32 devices in a mesh: ep: 8 (over z, x), tp: 4 (over y, core).
Axes of the slice: x: 2, y: 2, z: 4, core: 2. Of those that a mesh axis runs over, the one named last changes fastest.
Arguments:
- tokens: bfloat16 [1024, 2048], P('ep'), may hold values from -16 to 16
- routes: int32 [1024, 2], P('ep'), may hold values from 0 to 7, all different within a row; in each aligned block of 128 rows (0 to 127, 128 to 255, ...) at most 48 rows name the same one
- router: bfloat16 [2048, 8], replicated, may hold values from -0.125 to 0.125
- w_gate: bfloat16 [8, 2048, 2048], P('ep', None, 'tp'), may hold values from -0.125 to 0.125
- w_up: bfloat16 [8, 2048, 2048], P('ep', None, 'tp'), may hold values from -0.125 to 0.125
- w_down: bfloat16 [8, 2048, 2048], P('ep', 'tp'), may hold values from -0.125 to 0.125
- cotangent: bfloat16 [1024, 2048], P('ep'), may hold values from -6 to 6
Outputs:
- grad_tokens: bfloat16 [1024, 2048], P('ep', 'tp')
- grad_router: float32 [2048, 8], P('tp')
- grad_gate: float32 [8, 2048, 2048], P('ep', None, 'tp')
- grad_up: float32 [8, 2048, 2048], P('ep', None, 'tp')
- grad_down: float32 [8, 2048, 2048], P('ep', 'tp')
The draws below stay inside these ranges and needn't reach their ends.
Inputs may be any that keep to these rules, and one draw needn't show every extreme that they name: In each aligned block of 128 rows, no expert is named by more than 48 of the block's routes, a bound that some block reaches; a row names 2 different experts.
All inputs are finite; a program needn't handle non-finite values.
Results may differ from the reference program's by a relative error of at most 0.017.
Values may be sent and summed in bfloat16 or wider, within the bound.
A program may use at most 128 MiB of HBM per device.

```python
import math
import jax
import jax.numpy as jnp
import numpy as np
from jax import lax

D = 2048
FF = 2048
TOP_K = 2
TOK_DEV = 128
EXPERTS = 8
CAP = 48
TOKENS = 1024
N_EP = 8
N_TP = 4


def draw_tokens(key, part):
    key_rows = jax.random.fold_in(key, 11)
    key_vals = jax.random.fold_in(key, 23)
    values = jax.random.truncated_normal(key_vals, -4.0, 4.0, (TOKENS, D), jnp.float32)
    scales = jnp.exp(jax.random.uniform(key_rows, (TOKENS, 1), jnp.float32, math.log(0.5), math.log(4.0)))
    return (values * scales).astype(jnp.bfloat16)


def level_of(key, shape, shards, smallest, top_value):
    loudness = 1.0
    for axis_at, shards_of in shards:
        draws = jax.random.uniform(jax.random.fold_in(jax.random.fold_in(key, 6), axis_at), (shards_of,), jnp.float32, smallest / len(shards), top_value / len(shards))
        loudness = loudness * jnp.repeat(jnp.exp(draws), shape[axis_at] // shards_of).reshape((-1,) + (1,) * (len(shape) - 1 - axis_at))
    return loudness


def assign_block(rng, own, number, rows, number_of, top, limit, skew):
    order = jax.random.permutation(rng, number_of)
    crowded, common = load_shares(number_of, rows * top, limit, skew, True), load_shares(number_of, rows * top, limit, skew, False)
    places = jnp.arange(number_of)

    def named(tallies, rotation):
        used = int((tallies > 0).sum())
        fixed = max(1, used // 4)
        passed = fixed + (places - fixed + rotation * (used - fixed)) % max(1, number_of - fixed)
        return jnp.zeros((number_of,), jnp.int32).at[order[jnp.where(places < fixed, places, passed)]].set(jnp.asarray(tallies, jnp.int32))

    tallies = jnp.where(number % 4 == 0, named(crowded, number // 4), named(common, number - number // 4 - 1))
    mixed = jax.random.permutation(jax.random.fold_in(own, 3), number_of)
    giver, taker = mixed[0:number_of // 2 * 2:2], mixed[1:number_of // 2 * 2:2]
    slack = jnp.minimum(tallies[giver] - 1, limit - tallies[taker]) // 2
    slack = jnp.where((giver == order[0]) | (taker == order[0]) | (tallies[taker] == 0), 0, jnp.maximum(slack, 0))
    passed = jax.random.randint(jax.random.fold_in(own, 4), (number_of // 2,), 0, 1 << 20) % (slack + 1)
    tallies = tallies.at[giver].add(-passed).at[taker].add(passed)
    items = jnp.searchsorted(jnp.cumsum(tallies), jnp.arange(rows * top), side="right").astype(jnp.int32)
    listing = items.reshape(top, rows).T
    listing = listing[jax.random.permutation(jax.random.fold_in(own, 1), rows)]
    rotation = jax.random.randint(jax.random.fold_in(own, 2), (rows, 1), 0, top)
    return jnp.take_along_axis(listing, (jnp.arange(top)[None, :] + rotation) % top, axis=1)


def load_shares(amount, total, bound, lean, full):
    portions = [(1 << 20) // math.isqrt(standing ** lean) + 1 for standing in range(1, amount + 1)]
    largest = bound if full else min(bound, max(-(-total // amount), total * portions[0] // sum(portions)))
    least = 1 if total - largest >= amount - 1 else 0
    given, rest = [largest] + [least] * (amount - 1), total - largest - least * (amount - 1)
    while rest > 0:
        candidates = [i for i in range(1, amount) if given[i] < largest] or [i for i in range(1, amount) if given[i] < bound]
        whole, budget = sum([portions[i] for i in candidates]), rest
        for i in candidates:
            addition = min(bound - given[i], max(1, budget * portions[i] // whole), rest)
            given[i] = given[i] + addition
            rest = rest - addition
    return np.array(given)


def scatter_about(stream_key, shape, deviation, limit, split=(), kind=jnp.bfloat16):
    array = deviation * jax.random.normal(stream_key, shape, jnp.float32)
    if split:
        array = array * level_of(stream_key, shape, split, -0.22, 0.18)
    return jnp.clip(array, -limit, limit).astype(kind)


def setup_inputs(seed: int = 0) -> dict:
    key_list = jax.random.split(jax.random.key(seed), 8)
    tokens = draw_tokens(jax.random.fold_in(key_list[7], 71), 0)
    routes_keys = jax.random.split(jax.random.fold_in(key_list[1], 1), TOKENS // TOK_DEV)
    routes_turns = jax.random.permutation(jax.random.fold_in(key_list[1], 3), TOKENS // TOK_DEV)
    routes = jax.vmap(lambda own, number: assign_block(jax.random.fold_in(key_list[1], 2), own, number, TOK_DEV, EXPERTS, TOP_K, CAP, 2))(routes_keys, routes_turns).reshape((TOKENS, TOP_K))
    router = scatter_about(key_list[2], (D, EXPERTS), D ** -0.5, 0.125)
    w_gate = scatter_about(key_list[3], (EXPERTS, D, FF), D ** -0.5, 0.125, ((0, 8), (2, 4)))
    w_up = scatter_about(key_list[4], (EXPERTS, D, FF), D ** -0.5, 0.125, ((0, 8), (2, 4)))
    w_down = scatter_about(key_list[5], (EXPERTS, FF, D), FF ** -0.5, 0.125, ((0, 8), (1, 4)))
    cotangent = scatter_about(key_list[6], (TOKENS, D), 1.0, 6.0, ((0, 8),))
    return {"tokens": tokens, "routes": routes, "router": router, "w_gate": w_gate, "w_up": w_up, "w_down": w_down, "cotangent": cotangent}


clamp_limit = 7.0
sig_slope = 1.702


def reference(tokens, routes, router, w_gate, w_up, w_down, cotangent):
    highest = lax.Precision.HIGHEST
    assign_count = TOKENS * TOP_K
    logits = jnp.dot(tokens, router, preferred_element_type=jnp.float32)
    chosen = jnp.take_along_axis(logits, routes, axis=1)
    weights = 1.0 / jnp.sum(jnp.exp(chosen[:, None, :] - chosen[:, :, None]), axis=2)
    scaled = (weights[:, :, None] * cotangent[:, None, :].astype(jnp.float32)).astype(jnp.bfloat16)
    flat_routes = routes.reshape(N_EP, TOK_DEV * TOP_K)
    flat_hot = jax.nn.one_hot(flat_routes, EXPERTS, dtype=jnp.int32)
    earlier = jnp.cumsum(flat_hot, axis=1) - flat_hot
    position = jnp.sum(earlier * flat_hot, axis=2).reshape(-1).astype(jnp.int32)
    block_of = (jnp.arange(assign_count, dtype=jnp.int32) // (TOK_DEV * TOP_K)).astype(jnp.int32)
    slot_table = jnp.full((EXPERTS, N_EP, CAP), assign_count, jnp.int32)
    slot_table = slot_table.at[routes.reshape(-1).astype(jnp.int32), block_of, position].set(
        jnp.arange(assign_count, dtype=jnp.int32))
    slot_table = slot_table.reshape(EXPERTS, N_EP * CAP)
    token_pad = jnp.concatenate([tokens, jnp.zeros((1, D), jnp.bfloat16)], axis=0)
    scaled_pad = jnp.concatenate([scaled.reshape(assign_count, D), jnp.zeros((1, D), jnp.bfloat16)], axis=0)
    group_size = FF // N_TP

    def one_expert(packed):
        slots, gate_w, up_w, down_w = packed
        rows_in = token_pad[slots // TOP_K]
        cot_in = scaled_pad[slots]
        pre_gate = jnp.dot(rows_in, gate_w, preferred_element_type=jnp.float32)
        pre_up = jnp.dot(rows_in, up_w, preferred_element_type=jnp.float32)
        gate_clamped = jnp.minimum(pre_gate, clamp_limit)
        up_clamped = jnp.clip(pre_up, -clamp_limit, clamp_limit)
        sigmoid_gate = jax.nn.sigmoid(sig_slope * gate_clamped)
        gated_act = gate_clamped * sigmoid_gate
        activation = ((up_clamped + 1.0) * gated_act).astype(jnp.bfloat16)
        back_act = jnp.dot(cot_in, down_w.T, preferred_element_type=jnp.float32)
        shares = jnp.sum(activation.astype(jnp.float32) * back_act, axis=1)
        slope_term = sigmoid_gate + sig_slope * gated_act * (1.0 - sigmoid_gate)
        d_gate = jnp.where(pre_gate < clamp_limit, back_act * (up_clamped + 1.0) * slope_term, 0.0).astype(jnp.bfloat16)
        d_up = jnp.where(jnp.abs(pre_up) < clamp_limit, back_act * gated_act, 0.0).astype(jnp.bfloat16)
        grad_gate = jnp.dot(rows_in.T, d_gate, preferred_element_type=jnp.float32)
        grad_up = jnp.dot(rows_in.T, d_up, preferred_element_type=jnp.float32)
        grad_down = jnp.dot(activation.T, cot_in, preferred_element_type=jnp.float32)
        gate_groups = gate_w.astype(jnp.float32).reshape(D, N_TP, group_size)
        up_groups = up_w.astype(jnp.float32).reshape(D, N_TP, group_size)
        d_gate_groups = d_gate.astype(jnp.float32).reshape(-1, N_TP, group_size)
        d_up_groups = d_up.astype(jnp.float32).reshape(-1, N_TP, group_size)
        group_parts = jnp.einsum("rnf,dnf->nrd", d_gate_groups, gate_groups, precision=highest)
        group_parts = group_parts + jnp.einsum("rnf,dnf->nrd", d_up_groups, up_groups, precision=highest)
        rounded = lax.optimization_barrier(group_parts.astype(jnp.bfloat16)).astype(jnp.float32)
        input_rows = jnp.sum(rounded, axis=0)
        return grad_gate, grad_up, grad_down, input_rows, shares

    grad_gate, grad_up, grad_down, input_rows, shares = lax.map(one_expert, (slot_table, w_gate, w_up, w_down))
    flat_slots = slot_table.reshape(-1)
    grad_assign = jnp.zeros((assign_count + 1, D), jnp.float32).at[flat_slots].add(input_rows.reshape(-1, D))
    share_assign = jnp.zeros((assign_count + 1,), jnp.float32).at[flat_slots].add(shares.reshape(-1))
    from_experts = jnp.sum(grad_assign[:assign_count].reshape(TOKENS, TOP_K, D), axis=1)
    share_grid = share_assign[:assign_count].reshape(TOKENS, TOP_K)
    mixed_grad = share_grid - weights * jnp.sum(share_grid, axis=1, keepdims=True)
    d_logits = jnp.sum(jax.nn.one_hot(routes, EXPERTS, dtype=jnp.float32) * mixed_grad[:, :, None], axis=1)
    from_router = jnp.dot(d_logits, router.astype(jnp.float32).T, precision=highest)
    grad_tokens = (from_experts + from_router).astype(jnp.bfloat16)
    grad_router = jnp.dot(tokens.astype(jnp.float32).T, d_logits, precision=highest)
    return grad_tokens, grad_router, grad_gate, grad_up, grad_down
```

```python
import functools

import jax
import jax.numpy as jnp
from jax import lax
from jax.experimental import pallas as pl
from jax.experimental.pallas import tpu as pltpu
from jax.sharding import PartitionSpec as P

clamp_limit = 7.0
sig_slope = 1.702
MESH = pl.DeviceIdType.MESH
HIGH = lax.Precision.HIGHEST
NT = (((1,), (1,)), ((), ()))


def kernel(
    sizes,
    tok, rt, rout, cot, wg_hbm, wu_hbm, wd_hbm,
    gtok_out, grt_out, rows_out, cots_out, act_out, dg_out, du_out,
    wg, wu, wd, dsp, tok_send, cot_send, rows, cots, act, dg, du,
    part, cxr, ysend, yxr, ret_send, ret_recv,
    sh_part, shx, sh_tot, shr, rp_part, rpr,
    w_sem, o_sem, ep_s, ep_r, y_s, y_r, c_s, c_r,
    ca_s, ca_r, yb_s, yb_r, rb_s, rb_r, sa_s, sa_r, sb_s, sb_r, rp_s, rp_r,
):
    E, NTP, NY, C, T, D, F, H, groups = sizes
    me, tp = lax.axis_index("ep"), lax.axis_index("tp")
    y, c = tp // 2, lax.rem(tp, 2)
    f32, bf16 = jnp.float32, jnp.bfloat16

    def remote(src, dst, s, r, ep, tpi):
        return pltpu.make_async_remote_copy(
            src_ref=src, dst_ref=dst, send_sem=s, recv_sem=r,
            device_id=(ep, tpi), device_id_type=MESH)

    def up_ep(k):
        return lax.rem(me + k, E)

    def down_ep(k):
        return lax.rem(me + (E - k), E)

    def y_at(j):
        return lax.rem(y + j, NY)

    def cols_of(t):
        return pl.ds(pl.multiple_of(t * F, F), F)

    weight_copies = [
        pltpu.make_async_copy(a, b, w_sem.at[i])
        for i, (a, b) in enumerate(((wg_hbm, wg), (wu_hbm, wu), (wd_hbm, wd)))]
    for cp in weight_copies:
        cp.start()
    barrier = pltpu.get_barrier_semaphore()
    for k in range(1, E):
        pl.semaphore_signal(barrier, inc=1, device_id=(up_ep(k), tp), device_id_type=MESH)
    for j in range(1, NTP):
        pl.semaphore_signal(barrier, inc=1, device_id=(me, lax.rem(tp + j, NTP)), device_id_type=MESH)

    eid = lax.rem(lax.broadcasted_iota(jnp.int32, (E, T), 0) + me, E)
    hot = eid == rt[0:1, :]
    for i in range(1, rt.shape[0]):
        hot = hot | (eid == rt[i:i + 1, :])
    upper = (lax.broadcasted_iota(jnp.int32, (T, T), 0)
             < lax.broadcasted_iota(jnp.int32, (T, T), 1))
    pos = jnp.dot(hot.astype(f32).astype(bf16), upper.astype(f32).astype(bf16),
                  preferred_element_type=f32)
    posm = jnp.where(hot, pos, -1.0)
    crow = lax.broadcasted_iota(jnp.int32, (C, T), 0).astype(f32)
    for k in range(E):
        dsp[k * C:(k + 1) * C, :] = jnp.where(posm[k:k + 1, :] == crow, 1.0, 0.0).astype(bf16)
    tok_cols = tok[:, cols_of(tp)]
    cot_cols = cot[:, cols_of(tp)]
    tok_send[...] = jnp.dot(dsp[...], tok_cols, preferred_element_type=f32).astype(bf16)

    pl.semaphore_wait(barrier, E - 1 + NTP - 1)
    sends = []

    def send(*args):
        cp = remote(*args)
        cp.start()
        sends.append(cp)

    def blk(k):
        return pl.ds(k * C, C)

    for k in range(1, E):
        send(tok_send.at[blk(k), :], rows.at[blk(k), cols_of(tp)],
             ep_s.at[0], ep_r.at[0, k], up_ep(k), tp)

    perm = (lax.broadcasted_iota(jnp.int32, (E, E), 1)
            == lax.rem(lax.broadcasted_iota(jnp.int32, (E, E), 0) + me, E)).astype(f32)
    rout_rel = jnp.dot(perm.astype(bf16), rout[...], preferred_element_type=f32).astype(bf16)
    logits = lax.dot_general(rout_rel, tok[...], NT, preferred_element_type=f32)
    top = jnp.max(jnp.where(hot, logits, -1e30), axis=0, keepdims=True)
    ex = jnp.where(hot, jnp.exp(jnp.minimum(logits - top, 0.0)), 0.0)
    weight = ex / jnp.sum(ex, axis=0, keepdims=True)
    wcols = []
    for k in range(E):
        wcols.append(jnp.sum(jnp.where(posm[k:k + 1, :] == crow, weight[k:k + 1, :], 0.0),
                             axis=1, keepdims=True))
    for k in list(range(1, E)):
        raw = jnp.dot(dsp[blk(k), :], cot_cols, preferred_element_type=f32)
        cot_send[blk(k), :] = (wcols[k] * raw).astype(bf16)
    for k in range(1, E):
        send(cot_send.at[blk(k), :], cots.at[blk(k), cols_of(tp)],
             ep_s.at[1], ep_r.at[1, k], up_ep(k), tp)
    rows[0:C, :] = jnp.dot(dsp[0:C, :], tok[...], preferred_element_type=f32).astype(bf16)
    cots[0:C, :] = (wcols[0] * jnp.dot(dsp[0:C, :], cot[...], preferred_element_type=f32)).astype(bf16)

    bufs = (rows, cots)
    srcs = (tok_send, cot_send)

    def arrive(k):
        for a in range(2):
            buf = bufs[a]
            here = buf.at[blk(k), cols_of(tp)]
            remote(srcs[a].at[blk(k), :], here, ep_s.at[a], ep_r.at[a, k], me, tp).wait_recv()
            for j in range(1, NY):
                send(here, here, y_s.at[0], y_r.at[a, k, j], me, y_at(j) * 2 + c)
            send(here, here, c_s.at[0], c_r.at[a, k, 0], me, y * 2 + (1 - c))

    def pass_on(k):
        for a in range(2):
            for j in range(1, NY):
                t = lax.rem(y + (NY - j), NY) * 2 + c
                here = bufs[a].at[blk(k), cols_of(t)]
                remote(here, here, y_s.at[0], y_r.at[a, k, j], me, tp).wait_recv()
                send(here, here, c_s.at[0], c_r.at[a, k, j], me, y * 2 + (1 - c))

    def complete(k):
        for a in range(2):
            for j in range(NY):
                t = lax.rem(y + (NY - j), NY) * 2 + (1 - c)
                here = bufs[a].at[blk(k), cols_of(t)]
                remote(here, here, c_s.at[0], c_r.at[a, k, j], me, tp).wait_recv()

    tile = min(H, 256)
    ones = jnp.ones((8, tile), f32)

    def experts(k0, k1):
        r = pl.ds(k0 * C, (k1 - k0) * C)
        sums = [jnp.zeros((8, C), f32) for _ in range(k0, k1)]
        for n in range(0, H, tile):
            cn = slice(n, n + tile)
            pre_gate = jnp.dot(rows[r, :], wg[:, cn], preferred_element_type=f32)
            pre_up = jnp.dot(rows[r, :], wu[:, cn], preferred_element_type=f32)
            back = lax.dot_general(cots[r, :], wd[cn, :], NT, preferred_element_type=f32)
            g = jnp.minimum(pre_gate, clamp_limit)
            u1 = jnp.clip(pre_up, -clamp_limit, clamp_limit) + 1.0
            sg = jax.nn.sigmoid(sig_slope * g)
            ga = g * sg
            a = (u1 * ga).astype(bf16)
            act[r, cn] = a
            prod = a.astype(f32) * back
            slope = sg + sig_slope * ga * (1.0 - sg)
            dg[r, cn] = jnp.where(pre_gate < clamp_limit, back * u1 * slope, 0.0).astype(bf16)
            du[r, cn] = jnp.where(jnp.abs(pre_up) < clamp_limit, back * ga, 0.0).astype(bf16)
            for i in range(k1 - k0):
                sums[i] = sums[i] + lax.dot_general(
                    ones, prod[i * C:(i + 1) * C, :], NT, precision=HIGH, preferred_element_type=f32)
        for i in range(k1 - k0):
            sh_part[k0 + i, :, 0:C] = sums[i]

    def row_term(g, k0, k1):
        r = pl.ds(k0 * C, (k1 - k0) * C)
        for n in range(0, D, 512):
            part[r, n:n + 512] = (
                lax.dot_general(dg[r, :], wg[n:n + 512, :], NT, preferred_element_type=f32)
                + lax.dot_general(du[r, :], wu[n:n + 512, :], NT, preferred_element_type=f32)
            ).astype(bf16)
        for j in range(NY):
            send(part.at[r, cols_of(y_at(j) * 2 + (1 - c))], cxr.at[r, j * F:(j + 1) * F],
                 ca_s.at[0], ca_r.at[g, j], me, y * 2 + (1 - c))

    def chip_sum(g, k0, k1):
        r = pl.ds(k0 * C, (k1 - k0) * C)
        for j in list(range(1, NY)) + [0]:
            remote(part.at[r, cols_of(y_at(j) * 2 + (1 - c))], cxr.at[r, j * F:(j + 1) * F],
                   ca_s.at[0], ca_r.at[g, j], me, tp).wait_recv()
        for j in range(1, NY):
            f = slice((j - 1) * F, j * F)
            ysend[r, f] = (part[r, cols_of(y_at(j) * 2 + c)].astype(f32)
                           + cxr[r, j * F:(j + 1) * F].astype(f32)).astype(bf16)
            send(ysend.at[r, f], yxr.at[r, f], yb_s.at[0], yb_r.at[g, j], me, y_at(j) * 2 + c)

    def give_back(g, k0, k1):
        r = pl.ds(k0 * C, (k1 - k0) * C)
        total = part[r, cols_of(tp)].astype(f32) + cxr[r, 0:F].astype(f32)
        for j in range(1, NY):
            f = slice((j - 1) * F, j * F)
            remote(ysend.at[r, f], yxr.at[r, f], yb_s.at[0], yb_r.at[g, j], me, tp).wait_recv()
            total = total + yxr[r, f].astype(f32)
        ret_send[r, :] = total.astype(bf16)
        for k in range(max(k0, 1), k1):
            send(ret_send.at[blk(k), :], ret_recv.at[blk(k), :], rb_s.at[0], rb_r.at[k], down_ep(k), tp)

    half = groups[0][1]
    done = 0
    for k in range(1, E):
        arrive(k)
        if k > 1:
            pass_on(k - 1)
    pass_on(E - 1)
    for cp in weight_copies:
        cp.wait()
    for k in range(1, E):
        complete(k)
    out_copies = [pltpu.make_async_copy(a, b, o_sem.at[i]) for i, (a, b) in enumerate(
        ((rows, rows_out), (cots, cots_out), (act, act_out), (dg, dg_out), (du, du_out)))]
    for cp in out_copies[:2]:
        cp.start()
    for g, (k0, k1) in enumerate(groups):
        experts(k0, k1)
        row_term(g, k0, k1)
        if g > 0:
            chip_sum(g - 1, *groups[g - 1])
    for cp in out_copies[2:]:
        cp.start()
    for j in range(1, NTP):
        send(sh_part, shx.at[j], sa_s.at[0], sa_r.at[j], me, lax.rem(tp + j, NTP))
    last = len(groups) - 1
    chip_sum(last, *groups[last])
    for j in range(1, NTP):
        remote(sh_part, shx.at[j], sa_s.at[0], sa_r.at[j], me, tp).wait_recv()
    tot = sh_part[:, :, 0:C]
    for j in range(1, NTP):
        tot = tot + shx[j, :, :, 0:C]
    sh_tot[:, :, 0:C] = tot
    for k in range(1, E):
        send(sh_tot.at[k], shr.at[k], sb_s.at[0], sb_r.at[k], down_ep(k), tp)
    for g, (k0, k1) in enumerate(groups):
        give_back(g, k0, k1)
    srow = lax.broadcasted_iota(jnp.int32, (E, T), 0)
    share = jnp.zeros((E, T), f32)
    for k in range(E):
        if k == 0:
            sv = sh_tot[0, :, 0:C]
        else:
            remote(sh_tot.at[k], shr.at[k], sb_s.at[0], sb_r.at[k], me, tp).wait_recv()
            sv = shr[k, :, 0:C]
        got = jnp.dot(sv, dsp[blk(k), :].astype(f32), precision=HIGH, preferred_element_type=f32)
        share = jnp.where(srow == k, got[0:1, :], share)
    d_rel = share - weight * jnp.sum(share, axis=0, keepdims=True)
    d_rel = jnp.where(hot, d_rel, 0.0)
    d_abs = lax.dot_general(perm, d_rel, (((0,), (0,)), ((), ())), precision=HIGH,
                            preferred_element_type=f32)
    rp_part[...] = jnp.dot(d_abs, tok_cols.astype(f32), precision=HIGH, preferred_element_type=f32)
    for k in range(1, E):
        send(rp_part, rpr.at[k], rp_s.at[0], rp_r.at[k], up_ep(k), tp)
    from_router = lax.dot_general(
        d_abs, rout[:, cols_of(tp)].astype(f32), (((0,), (0,)), ((), ())), precision=HIGH,
        preferred_element_type=f32)
    ret_recv[0:C, :] = ret_send[0:C, :]
    for k in range(1, E):
        remote(ret_send.at[blk(k), :], ret_recv.at[blk(k), :], rb_s.at[0], rb_r.at[k], me, tp).wait_recv()
    from_experts = lax.dot_general(dsp[...], ret_recv[...], (((0,), (0,)), ((), ())),
                                   preferred_element_type=f32)
    gtok_out[...] = (from_experts + from_router).astype(bf16)
    rsum = rp_part[...]
    for k in range(1, E):
        remote(rp_part, rpr.at[k], rp_s.at[0], rp_r.at[k], me, tp).wait_recv()
        rsum = rsum + rpr[k]
    grt_out[...] = rsum
    for cp in sends:
        cp.wait_send()
    for cp in out_copies:
        cp.wait()


def on_device(tokens, routes, router, w_gate, w_up, w_down, cotangent):
    E = lax.axis_size("ep")
    NTP = lax.axis_size("tp")
    NY = NTP // 2
    T, D = tokens.shape
    H = w_gate.shape[2]
    F = D // NTP
    capacity = 3 * T * routes.shape[1] // (2 * E)
    C = -(-capacity // 16) * 16
    R = E * C
    groups = ((0, E // 2), (E // 2, E))
    G = len(groups)
    bf16, f32 = jnp.bfloat16, jnp.float32
    V = pltpu.VMEM
    dma = pltpu.SemaphoreType.DMA
    vmem = pl.BlockSpec(memory_space=pltpu.VMEM)
    hbm = pl.BlockSpec(memory_space=pl.ANY)
    gtok, grt, rows, cots, act, dg, du = pl.pallas_call(
        functools.partial(kernel, (E, NTP, NY, C, T, D, F, H, groups)),
        out_shape=[
            jax.ShapeDtypeStruct((T, F), bf16), jax.ShapeDtypeStruct((E, F), f32),
            jax.ShapeDtypeStruct((R, D), bf16), jax.ShapeDtypeStruct((R, D), bf16),
            jax.ShapeDtypeStruct((R, H), bf16), jax.ShapeDtypeStruct((R, H), bf16),
            jax.ShapeDtypeStruct((R, H), bf16)],
        in_specs=[vmem, vmem, vmem, vmem, hbm, hbm, hbm],
        out_specs=[vmem, vmem, hbm, hbm, hbm, hbm, hbm],
        scratch_shapes=[
            V((D, H), bf16), V((D, H), bf16), V((H, D), bf16),
            V((R, T), bf16), V((R, F), bf16), V((R, F), bf16),
            V((R, D), bf16), V((R, D), bf16),
            V((R, H), bf16), V((R, H), bf16), V((R, H), bf16),
            V((R, D), bf16), V((R, NY * F), bf16),
            V((R, max(NY - 1, 1) * F), bf16), V((R, max(NY - 1, 1) * F), bf16),
            V((R, F), bf16), V((R, F), bf16),
            V((E, 8, 128), f32), V((NTP, E, 8, 128), f32), V((E, 8, 128), f32), V((E, 8, 128), f32),
            V((E, F), f32), V((E, E, F), f32),
            dma((3,)), dma((5,)), dma((2,)), dma((2, E)), dma((1,)), dma((2, E, NY)),
            dma((1,)), dma((2, E, NY)),
            dma((1,)), dma((G, NY)), dma((1,)), dma((G, NY)), dma((1,)), dma((E,)),
            dma((1,)), dma((NTP,)), dma((1,)), dma((E,)), dma((1,)), dma((E,)),
        ],
        compiler_params=pltpu.CompilerParams(
            collective_id=0, has_side_effects=True, vmem_limit_bytes=60 * 1024 * 1024),
    )(tokens, routes.T, router.T, cotangent, w_gate[0], w_up[0], w_down[0])
    tn = (((0,), (0,)), ((), ()))
    grad_gate = lax.dot_general(rows, dg, tn, preferred_element_type=f32)[None]
    grad_up = lax.dot_general(rows, du, tn, preferred_element_type=f32)[None]
    grad_down = lax.dot_general(act, cots, tn, preferred_element_type=f32)[None]
    return (gtok, grt.T, grad_gate, grad_up, grad_down)


def solution(mesh):
    return jax.shard_map(
        on_device,
        mesh=mesh,
        in_specs=(
            P("ep", None),
            P("ep", None),
            P(),
            P("ep", None, "tp"),
            P("ep", None, "tp"),
            P("ep", "tp", None),
            P("ep", None),
        ),
        out_specs=(
            P("ep", "tp"),
            P("tp", None),
            P("ep", None, "tp"),
            P("ep", None, "tp"),
            P("ep", "tp", None),
        ),
        check_vma=False,
    )
```

```python
import functools

import jax
import jax.numpy as jnp
from jax import lax
from jax.experimental import pallas as pl
from jax.experimental.pallas import tpu as pltpu
from jax.sharding import PartitionSpec as P

clamp_limit = 7.0
sig_slope = 1.702
MESH = pl.DeviceIdType.MESH
HIGH = lax.Precision.HIGHEST
NT = (((1,), (1,)), ((), ()))


def kernel(
    sizes,
    tok, rt, rout, cot, wg_hbm, wu_hbm, wd_hbm,
    gtok_out, grt_out, rowst_out, cots_out, actt_out, dg_out, du_out,
    wg, wu, wd, dsp, tok_send, cot_send, rows, cots, rowst, actt, act, cg, cu, dg, du,
    part, cxr, ysend, yxr, ret_send, ret_recv,
    sh_part, shx, sh_tot, shr, rp_part, rpr,
    w_sem, o_sem, ep_s, ep_r, y_s, y_r, c_s, c_r,
    ca_s, ca_r, yb_s, yb_r, rb_s, rb_r, sa_s, sa_r, sb_s, sb_r, rp_s, rp_r,
):
    E, NTP, NY, C, T, D, F, H, groups = sizes
    me, tp = lax.axis_index("ep"), lax.axis_index("tp")
    y, c = tp // 2, lax.rem(tp, 2)
    f32, bf16 = jnp.float32, jnp.bfloat16

    def remote(src, dst, s, r, ep, tpi):
        return pltpu.make_async_remote_copy(
            src_ref=src, dst_ref=dst, send_sem=s, recv_sem=r,
            device_id=(ep, tpi), device_id_type=MESH)

    def up_ep(k):
        return lax.rem(me + k, E)

    def down_ep(k):
        return lax.rem(me + (E - k), E)

    def y_at(j):
        return lax.rem(y + j, NY)

    def cols_of(t):
        return pl.ds(pl.multiple_of(t * F, F), F)

    weight_copies = [
        pltpu.make_async_copy(a, b, w_sem.at[i])
        for i, (a, b) in enumerate(((wg_hbm, wg), (wu_hbm, wu), (wd_hbm, wd)))]
    for cp in weight_copies:
        cp.start()
    barrier = pltpu.get_barrier_semaphore()
    for k in range(1, E):
        pl.semaphore_signal(barrier, inc=1, device_id=(up_ep(k), tp), device_id_type=MESH)
    for j in range(1, NTP):
        pl.semaphore_signal(barrier, inc=1, device_id=(me, lax.rem(tp + j, NTP)), device_id_type=MESH)

    eid = lax.rem(lax.broadcasted_iota(jnp.int32, (E, T), 0) + me, E)
    hot = eid == rt[0:1, :]
    for i in range(1, rt.shape[0]):
        hot = hot | (eid == rt[i:i + 1, :])
    upper = (lax.broadcasted_iota(jnp.int32, (T, T), 0)
             < lax.broadcasted_iota(jnp.int32, (T, T), 1))
    pos = jnp.dot(hot.astype(f32).astype(bf16), upper.astype(f32).astype(bf16),
                  preferred_element_type=f32)
    posm = jnp.where(hot, pos, -1.0)
    crow = lax.broadcasted_iota(jnp.int32, (C, T), 0).astype(f32)
    for k in range(E):
        dsp[k * C:(k + 1) * C, :] = jnp.where(posm[k:k + 1, :] == crow, 1.0, 0.0).astype(bf16)
    tok_cols = tok[:, cols_of(tp)]
    cot_cols = cot[:, cols_of(tp)]
    tok_send[...] = jnp.dot(dsp[...], tok_cols, preferred_element_type=f32).astype(bf16)

    pl.semaphore_wait(barrier, E - 1 + NTP - 1)
    sends = []

    def send(*args):
        cp = remote(*args)
        cp.start()
        sends.append(cp)

    def blk(k):
        return pl.ds(k * C, C)

    for k in range(1, E):
        send(tok_send.at[blk(k), :], rows.at[blk(k), cols_of(tp)],
             ep_s.at[0], ep_r.at[0, k], up_ep(k), tp)

    perm = (lax.broadcasted_iota(jnp.int32, (E, E), 1)
            == lax.rem(lax.broadcasted_iota(jnp.int32, (E, E), 0) + me, E)).astype(f32)
    rout_rel = jnp.dot(perm.astype(bf16), rout[...], preferred_element_type=f32).astype(bf16)
    logits = lax.dot_general(rout_rel, tok[...], NT, preferred_element_type=f32)
    top = jnp.max(jnp.where(hot, logits, -1e30), axis=0, keepdims=True)
    ex = jnp.where(hot, jnp.exp(jnp.minimum(logits - top, 0.0)), 0.0)
    weight = ex / jnp.sum(ex, axis=0, keepdims=True)
    wcols = []
    for k in range(E):
        wcols.append(jnp.sum(jnp.where(posm[k:k + 1, :] == crow, weight[k:k + 1, :], 0.0),
                             axis=1, keepdims=True))
    for k in list(range(1, E)):
        raw = jnp.dot(dsp[blk(k), :], cot_cols, preferred_element_type=f32)
        cot_send[blk(k), :] = (wcols[k] * raw).astype(bf16)
    for k in range(1, E):
        send(cot_send.at[blk(k), :], cots.at[blk(k), cols_of(tp)],
             ep_s.at[1], ep_r.at[1, k], up_ep(k), tp)
    rows[0:C, :] = jnp.dot(dsp[0:C, :], tok[...], preferred_element_type=f32).astype(bf16)
    cots[0:C, :] = (wcols[0] * jnp.dot(dsp[0:C, :], cot[...], preferred_element_type=f32)).astype(bf16)

    bufs = (rows, cots)
    srcs = (tok_send, cot_send)

    def arrive(a, k):
        here = bufs[a].at[blk(k), cols_of(tp)]
        remote(srcs[a].at[blk(k), :], here, ep_s.at[a], ep_r.at[a, k], me, tp).wait_recv()
        for j in range(1, NY):
            send(here, here, y_s.at[0], y_r.at[a, k, j], me, y_at(j) * 2 + c)
        send(here, here, c_s.at[0], c_r.at[a, k, 0], me, y * 2 + (1 - c))

    def pass_on(a, k):
        for j in range(1, NY):
            t = lax.rem(y + (NY - j), NY) * 2 + c
            here = bufs[a].at[blk(k), cols_of(t)]
            remote(here, here, y_s.at[0], y_r.at[a, k, j], me, tp).wait_recv()
            send(here, here, c_s.at[0], c_r.at[a, k, j], me, y * 2 + (1 - c))

    def complete(a, k):
        for j in range(NY):
            t = lax.rem(y + (NY - j), NY) * 2 + (1 - c)
            here = bufs[a].at[blk(k), cols_of(t)]
            remote(here, here, c_s.at[0], c_r.at[a, k, j], me, tp).wait_recv()

    tile = min(H, 128)

    def forward(n):
        cn = slice(n, n + tile)
        pre_gate = jnp.dot(rows[...], wg[:, cn], preferred_element_type=f32)
        pre_up = jnp.dot(rows[...], wu[:, cn], preferred_element_type=f32)
        g = jnp.minimum(pre_gate, clamp_limit)
        u1 = jnp.clip(pre_up, -clamp_limit, clamp_limit) + 1.0
        sg = jax.nn.sigmoid(sig_slope * g)
        ga = g * sg
        a = (u1 * ga).astype(bf16)
        act[:, cn] = a
        actt[cn, :] = a.T
        slope = sg + sig_slope * ga * (1.0 - sg)
        cg[:, cn] = jnp.where(pre_gate < clamp_limit, u1 * slope, 0.0)
        cu[:, cn] = jnp.where(jnp.abs(pre_up) < clamp_limit, ga, 0.0)

    def backward(g, k0, k1):
        r = pl.ds(k0 * C, (k1 - k0) * C)
        total = None
        for n in range(0, H, tile):
            cn = slice(n, n + tile)
            back = lax.dot_general(cots[r, :], wd[cn, :], NT, preferred_element_type=f32)
            dg[r, cn] = (back * cg[r, cn]).astype(bf16)
            du[r, cn] = (back * cu[r, cn]).astype(bf16)
            prod = act[r, cn].astype(f32) * back
            total = prod if total is None else total + prod
        sh_part[g, :, 0:(k1 - k0) * C] = lax.dot_general(
            jnp.ones((8, tile), f32), total, NT, precision=HIGH, preferred_element_type=f32)

    def row_term(g, k0, k1):
        r = pl.ds(k0 * C, (k1 - k0) * C)

        def piece(t):
            d = pl.ds(pl.multiple_of(t * F, F), F)
            part[r, d] = (
                lax.dot_general(dg[r, :], wg[d, :], NT, preferred_element_type=f32)
                + lax.dot_general(du[r, :], wu[d, :], NT, preferred_element_type=f32)
            ).astype(bf16)

        order = list(range(1, NY)) + [0]
        for j in order:
            piece(y_at(j) * 2 + (1 - c))
            send(part.at[r, cols_of(y_at(j) * 2 + (1 - c))], cxr.at[r, j * F:(j + 1) * F],
                 ca_s.at[0], ca_r.at[g, j], me, y * 2 + (1 - c))
        for j in order:
            piece(y_at(j) * 2 + c)

    def chip_sum(g, k0, k1):
        r = pl.ds(k0 * C, (k1 - k0) * C)
        for j in list(range(1, NY)) + [0]:
            remote(part.at[r, cols_of(y_at(j) * 2 + (1 - c))], cxr.at[r, j * F:(j + 1) * F],
                   ca_s.at[0], ca_r.at[g, j], me, tp).wait_recv()
        for j in range(1, NY):
            f = slice((j - 1) * F, j * F)
            ysend[r, f] = (part[r, cols_of(y_at(j) * 2 + c)].astype(f32)
                           + cxr[r, j * F:(j + 1) * F].astype(f32)).astype(bf16)
            send(ysend.at[r, f], yxr.at[r, f], yb_s.at[0], yb_r.at[g, j], me, y_at(j) * 2 + c)

    def give_back(g, k0, k1):
        r = pl.ds(k0 * C, (k1 - k0) * C)
        total = part[r, cols_of(tp)].astype(f32) + cxr[r, 0:F].astype(f32)
        for j in range(1, NY):
            f = slice((j - 1) * F, j * F)
            remote(ysend.at[r, f], yxr.at[r, f], yb_s.at[0], yb_r.at[g, j], me, tp).wait_recv()
            total = total + yxr[r, f].astype(f32)
        ret_send[r, :] = total.astype(bf16)
        for k in range(max(k0, 1), k1):
            send(ret_send.at[blk(k), :], ret_recv.at[blk(k), :], rb_s.at[0], rb_r.at[k], down_ep(k), tp)

    out_copies = [pltpu.make_async_copy(a, b, o_sem.at[i]) for i, (a, b) in enumerate(
        ((rowst, rowst_out), (actt, actt_out), (cots, cots_out), (dg, dg_out), (du, du_out)))]
    items = [(a, k) for a in range(2) for k in range(1, E)]
    tiles = list(range(0, H, tile))
    per = max(1, -(-len(tiles) // max(1, E - 4)))
    for i, (a, k) in enumerate(items):
        arrive(a, k)
        if i > 0:
            pass_on(*items[i - 1])
        if (a, k) == (1, min(2, E - 1)):
            for cp in weight_copies:
                cp.wait()
            for kk in range(1, E):
                complete(0, kk)
        if a == 1 and k >= min(2, E - 1):
            for n in tiles[:per]:
                forward(n)
            tiles = tiles[per:]
    pass_on(*items[-1])
    for n in tiles:
        forward(n)
    nt = min(D, 256)
    for n in range(0, D, nt):
        rowst[n:n + nt, :] = rows[:, n:n + nt].T
    out_copies[0].start()
    out_copies[1].start()
    for g, (k0, k1) in enumerate(groups):
        for k in range(max(k0, 1), k1):
            complete(1, k)
        backward(g, k0, k1)
        row_term(g, k0, k1)
        if g > 0:
            chip_sum(g - 1, *groups[g - 1])
    for cp in out_copies[2:]:
        cp.start()
    last = len(groups) - 1
    for j in range(1, NTP):
        send(sh_part, shx.at[j], sa_s.at[0], sa_r.at[j], me, lax.rem(tp + j, NTP))
    chip_sum(last, *groups[last])
    for j in range(1, NTP):
        remote(sh_part, shx.at[j], sa_s.at[0], sa_r.at[j], me, tp).wait_recv()
    for g, (k0, k1) in enumerate(groups):
        tot = sh_part[g, :, 0:(k1 - k0) * C]
        for j in range(1, NTP):
            tot = tot + shx[j, g, :, 0:(k1 - k0) * C]
        for k in range(k0, k1):
            sh_tot[k, :, 0:C] = tot[:, (k - k0) * C:(k - k0 + 1) * C]
    for k in range(1, E):
        send(sh_tot.at[k], shr.at[k], sb_s.at[0], sb_r.at[k], down_ep(k), tp)
    for g, (k0, k1) in enumerate(groups):
        give_back(g, k0, k1)
    srow = lax.broadcasted_iota(jnp.int32, (E, T), 0)
    share = jnp.zeros((E, T), f32)
    for k in range(E):
        if k == 0:
            sv = sh_tot[0, :, 0:C]
        else:
            remote(sh_tot.at[k], shr.at[k], sb_s.at[0], sb_r.at[k], me, tp).wait_recv()
            sv = shr[k, :, 0:C]
        got = jnp.dot(sv, dsp[blk(k), :].astype(f32), precision=HIGH, preferred_element_type=f32)
        share = jnp.where(srow == k, got[0:1, :], share)
    d_rel = share - weight * jnp.sum(share, axis=0, keepdims=True)
    d_rel = jnp.where(hot, d_rel, 0.0)
    d_abs = lax.dot_general(perm, d_rel, (((0,), (0,)), ((), ())), precision=HIGH,
                            preferred_element_type=f32)
    rp_part[...] = jnp.dot(d_abs, tok_cols.astype(f32), precision=HIGH, preferred_element_type=f32)
    for k in range(1, E):
        send(rp_part, rpr.at[k], rp_s.at[0], rp_r.at[k], up_ep(k), tp)
    from_router = lax.dot_general(
        d_abs, rout[:, cols_of(tp)].astype(f32), (((0,), (0,)), ((), ())), precision=HIGH,
        preferred_element_type=f32)
    ret_recv[0:C, :] = ret_send[0:C, :]
    for k in range(1, E):
        remote(ret_send.at[blk(k), :], ret_recv.at[blk(k), :], rb_s.at[0], rb_r.at[k], me, tp).wait_recv()
    from_experts = lax.dot_general(dsp[...], ret_recv[...], (((0,), (0,)), ((), ())),
                                   preferred_element_type=f32)
    gtok_out[...] = (from_experts + from_router).astype(bf16)
    rsum = rp_part[...]
    for k in range(1, E):
        remote(rp_part, rpr.at[k], rp_s.at[0], rp_r.at[k], me, tp).wait_recv()
        rsum = rsum + rpr[k]
    grt_out[...] = rsum
    for cp in sends:
        cp.wait_send()
    for cp in out_copies:
        cp.wait()


def weight_grads(rowst, dg, du, actt, cots, gate_out, up_out, down_out):
    f32 = jnp.float32
    gate_out[0] = jnp.dot(rowst[...], dg[...], preferred_element_type=f32)
    up_out[0] = jnp.dot(rowst[...], du[...], preferred_element_type=f32)
    down_out[0] = jnp.dot(actt[...], cots[...], preferred_element_type=f32)


def on_device(tokens, routes, router, w_gate, w_up, w_down, cotangent):
    E = lax.axis_size("ep")
    NTP = lax.axis_size("tp")
    NY = NTP // 2
    T, D = tokens.shape
    H = w_gate.shape[2]
    F = D // NTP
    capacity = 3 * T * routes.shape[1] // (2 * E)
    C = -(-capacity // 16) * 16
    R = E * C
    groups = ((0, E // 2), (E // 2, E))
    G = len(groups)
    SW = -(-max(b - a for a, b in groups) * C // 128) * 128
    bf16, f32 = jnp.bfloat16, jnp.float32
    V = pltpu.VMEM
    dma = pltpu.SemaphoreType.DMA
    vmem = pl.BlockSpec(memory_space=pltpu.VMEM)
    hbm = pl.BlockSpec(memory_space=pl.ANY)
    gtok, grt, rowst, cots, actt, dg, du = pl.pallas_call(
        functools.partial(kernel, (E, NTP, NY, C, T, D, F, H, groups)),
        out_shape=[
            jax.ShapeDtypeStruct((T, F), bf16), jax.ShapeDtypeStruct((E, F), f32),
            jax.ShapeDtypeStruct((D, R), bf16), jax.ShapeDtypeStruct((R, D), bf16),
            jax.ShapeDtypeStruct((H, R), bf16), jax.ShapeDtypeStruct((R, H), bf16),
            jax.ShapeDtypeStruct((R, H), bf16)],
        in_specs=[vmem, vmem, vmem, vmem, hbm, hbm, hbm],
        out_specs=[vmem, vmem, hbm, hbm, hbm, hbm, hbm],
        scratch_shapes=[
            V((D, H), bf16), V((D, H), bf16), V((H, D), bf16),
            V((R, T), bf16), V((R, F), bf16), V((R, F), bf16),
            V((R, D), bf16), V((R, D), bf16), V((D, R), bf16), V((H, R), bf16),
            V((R, H), bf16), V((R, H), f32), V((R, H), f32), V((R, H), bf16), V((R, H), bf16),
            V((R, D), bf16), V((R, NY * F), bf16),
            V((R, max(NY - 1, 1) * F), bf16), V((R, max(NY - 1, 1) * F), bf16),
            V((R, F), bf16), V((R, F), bf16),
            V((G, 8, SW), f32), V((NTP, G, 8, SW), f32), V((E, 8, 128), f32), V((E, 8, 128), f32),
            V((E, F), f32), V((E, E, F), f32),
            dma((3,)), dma((5,)), dma((2,)), dma((2, E)), dma((1,)), dma((2, E, NY)),
            dma((1,)), dma((2, E, NY)),
            dma((1,)), dma((G, NY)), dma((1,)), dma((G, NY)), dma((1,)), dma((E,)),
            dma((1,)), dma((NTP,)), dma((1,)), dma((E,)), dma((1,)), dma((E,)),
        ],
        compiler_params=pltpu.CompilerParams(
            collective_id=0, has_side_effects=True, vmem_limit_bytes=60 * 1024 * 1024),
    )(tokens, routes.T, router.T, cotangent, w_gate[0], w_up[0], w_down[0])
    steps = 8
    dt, ht = D // steps, H // steps
    grad_gate, grad_up, grad_down = pl.pallas_call(
        weight_grads,
        grid=(steps,),
        out_shape=[jax.ShapeDtypeStruct((1, D, H), f32), jax.ShapeDtypeStruct((1, D, H), f32),
                   jax.ShapeDtypeStruct((1, H, D), f32)],
        in_specs=[
            pl.BlockSpec((dt, R), lambda i: (i, 0)), pl.BlockSpec((R, H), lambda i: (0, 0)),
            pl.BlockSpec((R, H), lambda i: (0, 0)), pl.BlockSpec((ht, R), lambda i: (i, 0)),
            pl.BlockSpec((R, D), lambda i: (0, 0))],
        out_specs=[
            pl.BlockSpec((1, dt, H), lambda i: (0, i, 0)), pl.BlockSpec((1, dt, H), lambda i: (0, i, 0)),
            pl.BlockSpec((1, ht, D), lambda i: (0, i, 0))],
        compiler_params=pltpu.CompilerParams(dimension_semantics=("arbitrary",)),
    )(rowst, dg, du, actt, cots)
    return (gtok, grt.T, grad_gate, grad_up, grad_down)


def solution(mesh):
    return jax.shard_map(
        on_device,
        mesh=mesh,
        in_specs=(
            P("ep", None),
            P("ep", None),
            P(),
            P("ep", None, "tp"),
            P("ep", None, "tp"),
            P("ep", "tp", None),
            P("ep", None),
        ),
        out_specs=(
            P("ep", "tp"),
            P("tp", None),
            P("ep", None, "tp"),
            P("ep", None, "tp"),
            P("ep", "tp", None),
        ),
        check_vma=False,
    )
```

```python
import functools

import jax
import jax.numpy as jnp
from jax import lax
from jax.experimental import pallas as pl
from jax.experimental.pallas import tpu as pltpu
from jax.sharding import PartitionSpec as P

clamp_limit = 7.0
sig_slope = 1.702
WINDOW = 3
MESH = pl.DeviceIdType.MESH
HIGH = lax.Precision.HIGHEST
NT = (((1,), (1,)), ((), ()))


def kernel(
    sizes,
    tok, rt, rout, cot, wg_hbm, wu_hbm, wd_hbm,
    gtok_out, grt_out, rowst_out, cots_out, actt_out, dg_out, du_out,
    wg, wu, wd, dsp, tok_send, cot_send, rows, cots, rowst, actt, act, cg, cu, dg, du,
    part, cxr, ysend, yxr, ret_send, ret_recv,
    sh_part, shx, sh_tot, shr, rp_part, rpr,
    w_sem, o_sem, ep_s, ep_r, y_s, y_r, c_s, c_r,
    ca_s, ca_r, yb_s, yb_r, rb_s, rb_r, sa_s, sa_r, sb_s, sb_r, rp_s, rp_r,
):
    E, NTP, NY, C, T, D, F, H, groups = sizes
    me, tp = lax.axis_index("ep"), lax.axis_index("tp")
    y, c = tp // 2, lax.rem(tp, 2)
    f32, bf16 = jnp.float32, jnp.bfloat16

    def remote(src, dst, s, r, ep, tpi):
        return pltpu.make_async_remote_copy(
            src_ref=src, dst_ref=dst, send_sem=s, recv_sem=r,
            device_id=(ep, tpi), device_id_type=MESH)

    def up_ep(k):
        return lax.rem(me + k, E)

    def down_ep(k):
        return lax.rem(me + (E - k), E)

    def y_at(j):
        return lax.rem(y + j, NY)

    def cols_of(t):
        return pl.ds(pl.multiple_of(t * F, F), F)

    weight_copies = [
        pltpu.make_async_copy(a, b, w_sem.at[i])
        for i, (a, b) in enumerate(((wg_hbm, wg), (wu_hbm, wu), (wd_hbm, wd)))]
    for cp in weight_copies:
        cp.start()
    barrier = pltpu.get_barrier_semaphore()
    for k in range(1, E):
        pl.semaphore_signal(barrier, inc=1, device_id=(up_ep(k), tp), device_id_type=MESH)
    for j in range(1, NTP):
        pl.semaphore_signal(barrier, inc=1, device_id=(me, lax.rem(tp + j, NTP)), device_id_type=MESH)

    eid = lax.rem(lax.broadcasted_iota(jnp.int32, (E, T), 0) + me, E)
    hot = eid == rt[0:1, :]
    for i in range(1, rt.shape[0]):
        hot = hot | (eid == rt[i:i + 1, :])
    upper = (lax.broadcasted_iota(jnp.int32, (T, T), 0)
             < lax.broadcasted_iota(jnp.int32, (T, T), 1))
    pos = jnp.dot(hot.astype(f32).astype(bf16), upper.astype(f32).astype(bf16),
                  preferred_element_type=f32)
    posm = jnp.where(hot, pos, -1.0)
    crow = lax.broadcasted_iota(jnp.int32, (C, T), 0).astype(f32)
    for k in range(E):
        dsp[k * C:(k + 1) * C, :] = jnp.where(posm[k:k + 1, :] == crow, 1.0, 0.0).astype(bf16)
    tok_cols = tok[:, cols_of(tp)]
    cot_cols = cot[:, cols_of(tp)]
    tok_send[...] = jnp.dot(dsp[...], tok_cols, preferred_element_type=f32).astype(bf16)

    pl.semaphore_wait(barrier, E - 1 + NTP - 1)
    sends = []

    def send(*args):
        cp = remote(*args)
        cp.start()
        sends.append(cp)

    def blk(k):
        return pl.ds(k * C, C)

    bufs = (rows, cots)
    srcs = (tok_send, cot_send)
    items = [(a, k) for a in range(2) for k in range(1, E)]
    window = min(WINDOW, E - 1)

    def send_out(a, k):
        send(srcs[a].at[blk(k), :], bufs[a].at[blk(k), cols_of(tp)],
             ep_s.at[a], ep_r.at[a, k], up_ep(k), tp)

    for a, k in items[:window]:
        send_out(a, k)

    perm = (lax.broadcasted_iota(jnp.int32, (E, E), 1)
            == lax.rem(lax.broadcasted_iota(jnp.int32, (E, E), 0) + me, E)).astype(f32)
    rout_rel = jnp.dot(perm.astype(bf16), rout[...], preferred_element_type=f32).astype(bf16)
    logits = lax.dot_general(rout_rel, tok[...], NT, preferred_element_type=f32)
    top = jnp.max(jnp.where(hot, logits, -1e30), axis=0, keepdims=True)
    ex = jnp.where(hot, jnp.exp(jnp.minimum(logits - top, 0.0)), 0.0)
    weight = ex / jnp.sum(ex, axis=0, keepdims=True)
    wcols = []
    for k in range(E):
        wcols.append(jnp.sum(jnp.where(posm[k:k + 1, :] == crow, weight[k:k + 1, :], 0.0),
                             axis=1, keepdims=True))
    for k in list(range(1, E)):
        raw = jnp.dot(dsp[blk(k), :], cot_cols, preferred_element_type=f32)
        cot_send[blk(k), :] = (wcols[k] * raw).astype(bf16)
    rows[0:C, :] = jnp.dot(dsp[0:C, :], tok[...], preferred_element_type=f32).astype(bf16)
    cots[0:C, :] = (wcols[0] * jnp.dot(dsp[0:C, :], cot[...], preferred_element_type=f32)).astype(bf16)

    def arrive(a, k):
        here = bufs[a].at[blk(k), cols_of(tp)]
        remote(srcs[a].at[blk(k), :], here, ep_s.at[a], ep_r.at[a, k], me, tp).wait_recv()
        for j in range(1, NY):
            send(here, here, y_s.at[0], y_r.at[a, k, j], me, y_at(j) * 2 + c)
        send(here, here, c_s.at[0], c_r.at[a, k, 0], me, y * 2 + (1 - c))

    def pass_on(a, k):
        for j in range(1, NY):
            t = lax.rem(y + (NY - j), NY) * 2 + c
            here = bufs[a].at[blk(k), cols_of(t)]
            remote(here, here, y_s.at[0], y_r.at[a, k, j], me, tp).wait_recv()
            send(here, here, c_s.at[0], c_r.at[a, k, j], me, y * 2 + (1 - c))

    def complete(a, k):
        for j in range(NY):
            t = lax.rem(y + (NY - j), NY) * 2 + (1 - c)
            here = bufs[a].at[blk(k), cols_of(t)]
            remote(here, here, c_s.at[0], c_r.at[a, k, j], me, tp).wait_recv()

    tile = min(H, 128)

    def forward(n):
        cn = slice(n, n + tile)
        pre_gate = jnp.dot(rows[...], wg[:, cn], preferred_element_type=f32)
        pre_up = jnp.dot(rows[...], wu[:, cn], preferred_element_type=f32)
        g = jnp.minimum(pre_gate, clamp_limit)
        u1 = jnp.clip(pre_up, -clamp_limit, clamp_limit) + 1.0
        sg = jax.nn.sigmoid(sig_slope * g)
        ga = g * sg
        a = (u1 * ga).astype(bf16)
        act[:, cn] = a
        actt[cn, :] = a.T
        slope = sg + sig_slope * ga * (1.0 - sg)
        cg[:, cn] = jnp.where(pre_gate < clamp_limit, u1 * slope, 0.0)
        cu[:, cn] = jnp.where(jnp.abs(pre_up) < clamp_limit, ga, 0.0)

    def backward(g, k0, k1):
        r = pl.ds(k0 * C, (k1 - k0) * C)
        total = None
        for n in range(0, H, tile):
            cn = slice(n, n + tile)
            back = lax.dot_general(cots[r, :], wd[cn, :], NT, preferred_element_type=f32)
            dg[r, cn] = (back * cg[r, cn]).astype(bf16)
            du[r, cn] = (back * cu[r, cn]).astype(bf16)
            prod = act[r, cn].astype(f32) * back
            total = prod if total is None else total + prod
        sh_part[g, :, 0:(k1 - k0) * C] = lax.dot_general(
            jnp.ones((8, tile), f32), total, NT, precision=HIGH, preferred_element_type=f32)

    def row_term(g, k0, k1):
        r = pl.ds(k0 * C, (k1 - k0) * C)

        def piece(t):
            d = pl.ds(pl.multiple_of(t * F, F), F)
            part[r, d] = (
                lax.dot_general(dg[r, :], wg[d, :], NT, preferred_element_type=f32)
                + lax.dot_general(du[r, :], wu[d, :], NT, preferred_element_type=f32)
            ).astype(bf16)

        order = list(range(1, NY)) + [0]
        for j in order:
            piece(y_at(j) * 2 + (1 - c))
            send(part.at[r, cols_of(y_at(j) * 2 + (1 - c))], cxr.at[r, j * F:(j + 1) * F],
                 ca_s.at[0], ca_r.at[g, j], me, y * 2 + (1 - c))
        for j in order:
            piece(y_at(j) * 2 + c)

    def chip_sum(g, k0, k1):
        r = pl.ds(k0 * C, (k1 - k0) * C)
        for j in list(range(1, NY)) + [0]:
            remote(part.at[r, cols_of(y_at(j) * 2 + (1 - c))], cxr.at[r, j * F:(j + 1) * F],
                   ca_s.at[0], ca_r.at[g, j], me, tp).wait_recv()
        for j in range(1, NY):
            f = slice((j - 1) * F, j * F)
            ysend[r, f] = (part[r, cols_of(y_at(j) * 2 + c)].astype(f32)
                           + cxr[r, j * F:(j + 1) * F].astype(f32)).astype(bf16)
            send(ysend.at[r, f], yxr.at[r, f], yb_s.at[0], yb_r.at[g, j], me, y_at(j) * 2 + c)

    def give_back(g, k0, k1):
        r = pl.ds(k0 * C, (k1 - k0) * C)
        total = part[r, cols_of(tp)].astype(f32) + cxr[r, 0:F].astype(f32)
        for j in range(1, NY):
            f = slice((j - 1) * F, j * F)
            remote(ysend.at[r, f], yxr.at[r, f], yb_s.at[0], yb_r.at[g, j], me, tp).wait_recv()
            total = total + yxr[r, f].astype(f32)
        ret_send[r, :] = total.astype(bf16)
        for k in range(max(k0, 1), k1):
            send(ret_send.at[blk(k), :], ret_recv.at[blk(k), :], rb_s.at[0], rb_r.at[k], down_ep(k), tp)

    out_copies = [pltpu.make_async_copy(a, b, o_sem.at[i]) for i, (a, b) in enumerate(
        ((rowst, rowst_out), (actt, actt_out), (cots, cots_out), (dg, dg_out), (du, du_out)))]
    tiles = list(range(0, H, tile))
    per = max(1, -(-len(tiles) // max(1, E - 4)))
    for i, (a, k) in enumerate(items):
        arrive(a, k)
        if i + window < len(items):
            send_out(*items[i + window])
        if i > 0:
            pass_on(*items[i - 1])
        if (a, k) == (1, min(2, E - 1)):
            for cp in weight_copies:
                cp.wait()
            for kk in range(1, E):
                complete(0, kk)
        if a == 1 and k >= min(2, E - 1):
            for n in tiles[:per]:
                forward(n)
            tiles = tiles[per:]
    pass_on(*items[-1])
    for n in tiles:
        forward(n)
    nt = min(D, 256)
    for n in range(0, D, nt):
        rowst[n:n + nt, :] = rows[:, n:n + nt].T
    out_copies[0].start()
    out_copies[1].start()
    for g, (k0, k1) in enumerate(groups):
        for k in range(max(k0, 1), k1):
            complete(1, k)
        backward(g, k0, k1)
        row_term(g, k0, k1)
        if g > 0:
            chip_sum(g - 1, *groups[g - 1])
    for cp in out_copies[2:]:
        cp.start()
    last = len(groups) - 1
    for j in range(1, NTP):
        send(sh_part, shx.at[j], sa_s.at[0], sa_r.at[j], me, lax.rem(tp + j, NTP))
    chip_sum(last, *groups[last])
    for j in range(1, NTP):
        remote(sh_part, shx.at[j], sa_s.at[0], sa_r.at[j], me, tp).wait_recv()
    for g, (k0, k1) in enumerate(groups):
        tot = sh_part[g, :, 0:(k1 - k0) * C]
        for j in range(1, NTP):
            tot = tot + shx[j, g, :, 0:(k1 - k0) * C]
        for k in range(k0, k1):
            sh_tot[k, :, 0:C] = tot[:, (k - k0) * C:(k - k0 + 1) * C]
    for k in range(1, E):
        send(sh_tot.at[k], shr.at[k], sb_s.at[0], sb_r.at[k], down_ep(k), tp)
    for g, (k0, k1) in enumerate(groups):
        give_back(g, k0, k1)
    srow = lax.broadcasted_iota(jnp.int32, (E, T), 0)
    share = jnp.zeros((E, T), f32)
    for k in range(E):
        if k == 0:
            sv = sh_tot[0, :, 0:C]
        else:
            remote(sh_tot.at[k], shr.at[k], sb_s.at[0], sb_r.at[k], me, tp).wait_recv()
            sv = shr[k, :, 0:C]
        got = jnp.dot(sv, dsp[blk(k), :].astype(f32), precision=HIGH, preferred_element_type=f32)
        share = jnp.where(srow == k, got[0:1, :], share)
    d_rel = share - weight * jnp.sum(share, axis=0, keepdims=True)
    d_rel = jnp.where(hot, d_rel, 0.0)
    d_abs = lax.dot_general(perm, d_rel, (((0,), (0,)), ((), ())), precision=HIGH,
                            preferred_element_type=f32)
    rp_part[...] = jnp.dot(d_abs, tok_cols.astype(f32), precision=HIGH, preferred_element_type=f32)
    for k in range(1, E):
        send(rp_part, rpr.at[k], rp_s.at[0], rp_r.at[k], up_ep(k), tp)
    from_router = lax.dot_general(
        d_abs, rout[:, cols_of(tp)].astype(f32), (((0,), (0,)), ((), ())), precision=HIGH,
        preferred_element_type=f32)
    ret_recv[0:C, :] = ret_send[0:C, :]
    for k in range(1, E):
        remote(ret_send.at[blk(k), :], ret_recv.at[blk(k), :], rb_s.at[0], rb_r.at[k], me, tp).wait_recv()
    from_experts = lax.dot_general(dsp[...], ret_recv[...], (((0,), (0,)), ((), ())),
                                   preferred_element_type=f32)
    gtok_out[...] = (from_experts + from_router).astype(bf16)
    rsum = rp_part[...]
    for k in range(1, E):
        remote(rp_part, rpr.at[k], rp_s.at[0], rp_r.at[k], me, tp).wait_recv()
        rsum = rsum + rpr[k]
    grt_out[...] = rsum
    for cp in sends:
        cp.wait_send()
    for cp in out_copies:
        cp.wait()


def weight_grads(rowst, dg, du, actt, cots, gate_out, up_out, down_out):
    f32 = jnp.float32
    gate_out[0] = jnp.dot(rowst[...], dg[...], preferred_element_type=f32)
    up_out[0] = jnp.dot(rowst[...], du[...], preferred_element_type=f32)
    down_out[0] = jnp.dot(actt[...], cots[...], preferred_element_type=f32)


def on_device(tokens, routes, router, w_gate, w_up, w_down, cotangent):
    E = lax.axis_size("ep")
    NTP = lax.axis_size("tp")
    NY = NTP // 2
    T, D = tokens.shape
    H = w_gate.shape[2]
    F = D // NTP
    capacity = 3 * T * routes.shape[1] // (2 * E)
    C = -(-capacity // 16) * 16
    R = E * C
    groups = ((0, E // 2), (E // 2, E))
    G = len(groups)
    SW = -(-max(b - a for a, b in groups) * C // 128) * 128
    bf16, f32 = jnp.bfloat16, jnp.float32
    V = pltpu.VMEM
    dma = pltpu.SemaphoreType.DMA
    vmem = pl.BlockSpec(memory_space=pltpu.VMEM)
    hbm = pl.BlockSpec(memory_space=pl.ANY)
    gtok, grt, rowst, cots, actt, dg, du = pl.pallas_call(
        functools.partial(kernel, (E, NTP, NY, C, T, D, F, H, groups)),
        out_shape=[
            jax.ShapeDtypeStruct((T, F), bf16), jax.ShapeDtypeStruct((E, F), f32),
            jax.ShapeDtypeStruct((D, R), bf16), jax.ShapeDtypeStruct((R, D), bf16),
            jax.ShapeDtypeStruct((H, R), bf16), jax.ShapeDtypeStruct((R, H), bf16),
            jax.ShapeDtypeStruct((R, H), bf16)],
        in_specs=[vmem, vmem, vmem, vmem, hbm, hbm, hbm],
        out_specs=[vmem, vmem, hbm, hbm, hbm, hbm, hbm],
        scratch_shapes=[
            V((D, H), bf16), V((D, H), bf16), V((H, D), bf16),
            V((R, T), bf16), V((R, F), bf16), V((R, F), bf16),
            V((R, D), bf16), V((R, D), bf16), V((D, R), bf16), V((H, R), bf16),
            V((R, H), bf16), V((R, H), f32), V((R, H), f32), V((R, H), bf16), V((R, H), bf16),
            V((R, D), bf16), V((R, NY * F), bf16),
            V((R, max(NY - 1, 1) * F), bf16), V((R, max(NY - 1, 1) * F), bf16),
            V((R, F), bf16), V((R, F), bf16),
            V((G, 8, SW), f32), V((NTP, G, 8, SW), f32), V((E, 8, 128), f32), V((E, 8, 128), f32),
            V((E, F), f32), V((E, E, F), f32),
            dma((3,)), dma((5,)), dma((2,)), dma((2, E)), dma((1,)), dma((2, E, NY)),
            dma((1,)), dma((2, E, NY)),
            dma((1,)), dma((G, NY)), dma((1,)), dma((G, NY)), dma((1,)), dma((E,)),
            dma((1,)), dma((NTP,)), dma((1,)), dma((E,)), dma((1,)), dma((E,)),
        ],
        compiler_params=pltpu.CompilerParams(
            collective_id=0, has_side_effects=True, vmem_limit_bytes=60 * 1024 * 1024),
    )(tokens, routes.T, router.T, cotangent, w_gate[0], w_up[0], w_down[0])
    steps = 8
    dt, ht = D // steps, H // steps
    grad_gate, grad_up, grad_down = pl.pallas_call(
        weight_grads,
        grid=(steps,),
        out_shape=[jax.ShapeDtypeStruct((1, D, H), f32), jax.ShapeDtypeStruct((1, D, H), f32),
                   jax.ShapeDtypeStruct((1, H, D), f32)],
        in_specs=[
            pl.BlockSpec((dt, R), lambda i: (i, 0)), pl.BlockSpec((R, H), lambda i: (0, 0)),
            pl.BlockSpec((R, H), lambda i: (0, 0)), pl.BlockSpec((ht, R), lambda i: (i, 0)),
            pl.BlockSpec((R, D), lambda i: (0, 0))],
        out_specs=[
            pl.BlockSpec((1, dt, H), lambda i: (0, i, 0)), pl.BlockSpec((1, dt, H), lambda i: (0, i, 0)),
            pl.BlockSpec((1, ht, D), lambda i: (0, i, 0))],
        compiler_params=pltpu.CompilerParams(dimension_semantics=("arbitrary",)),
    )(rowst, dg, du, actt, cots)
    return (gtok, grt.T, grad_gate, grad_up, grad_down)


def solution(mesh):
    return jax.shard_map(
        on_device,
        mesh=mesh,
        in_specs=(
            P("ep", None),
            P("ep", None),
            P(),
            P("ep", None, "tp"),
            P("ep", None, "tp"),
            P("ep", "tp", None),
            P("ep", None),
        ),
        out_specs=(
            P("ep", "tp"),
            P("tp", None),
            P("ep", None, "tp"),
            P("ep", None, "tp"),
            P("ep", "tp", None),
        ),
        check_vma=False,
    )
```
